32 devices in a mesh: ep: 32 (over z, y, x, core).
Axes of the slice: x: 2, y: 2, z: 4, core: 2. Of those that a mesh axis runs over, the one named last changes fastest.
Arguments:
- tokens: bfloat16 [128, 2048], P('ep'), may hold values from -6 to 6
- recurrent_state: float32 [128, 8, 128, 128], P('ep'), may hold values from -4 to 4
- query_weight: bfloat16 [2048, 1024], P(None, 'ep'), may hold values from -0.125 to 0.125
- forget_weight: bfloat16 [2048, 1024], P(None, 'ep'), may hold values from -0.125 to 0.125
- input_weight: bfloat16 [2048, 1024], P(None, 'ep'), may hold values from -0.125 to 0.125
- outgate_weight: bfloat16 [2048, 1024], P(None, 'ep'), may hold values from -0.125 to 0.125
- lower_bound: float32 [1024], replicated, may hold values from 0 to 0.9
- head_gain: float32 [128], replicated, may hold values from 0.1 to 1.9
- mixout_weight: bfloat16 [1024, 2048], P(None, 'ep'), may hold values from -0.1875 to 0.1875
- first_gain: float32 [2048], replicated, may hold values from 0.1 to 1.9
- first_bias: float32 [2048], replicated, may hold values from -1.5 to 1.5
- router_weight: bfloat16 [2048, 8], replicated, may hold values from -0.125 to 0.125
- branch_vector: bfloat16 [2048], replicated, may hold values from -0.125 to 0.125
- dense_gate_weight: bfloat16 [2048, 5632], P(None, 'ep'), may hold values from -0.125 to 0.125
- dense_up_weight: bfloat16 [2048, 5632], P(None, 'ep'), may hold values from -0.125 to 0.125
- dense_down_weight: bfloat16 [5632, 2048], P('ep'), may hold values from -0.078125 to 0.078125
- expert_gate_weight: bfloat16 [2048, 57344], P(None, 'ep'), may hold values from -0.125 to 0.125
- expert_up_weight: bfloat16 [2048, 57344], P(None, 'ep'), may hold values from -0.125 to 0.125
- expert_down_weight: bfloat16 [57344, 2048], P('ep'), may hold values from -0.0625 to 0.0625
- second_gain: float32 [2048], replicated, may hold values from 0.1 to 1.9
- second_bias: float32 [2048], replicated, may hold values from -1.5 to 1.5
- routes: int32 [128, 2], replicated, may hold values from 0 to 7, all different within a row; in each aligned block of 4 rows (0 to 3, 4 to 7, ...) at most 2 rows name the same one
Outputs:
- output: bfloat16 [128, 2048], P('ep')
- new_state: float32 [128, 8, 128, 128], P('ep')
The draws below stay inside these ranges and needn't reach their ends.
Inputs may be any that keep to these rules, and one draw needn't show every extreme that they name: `routes`: each row names two different experts; in the rows of one device no expert is named more than 2 times, a bound that some block reaches in some device's rows.
All inputs are finite; a program needn't handle non-finite values.
Results may differ from the reference program's by a relative error of at most 0.0095.
Values may be sent and summed in bfloat16 or wider, within the bound.
No kernel may reach another device: no remote copies, remote signals or barrier semaphores. Data moves between devices by JAX's collectives and lax.ppermute only.
A program may use at most 64 MiB of HBM per device.

```python
import math
import jax
import jax.numpy as jnp
import numpy as np
from jax import lax

D = 2048
HGW = 1024
DK = 128
HEADS = 8
EXPERTS = 8
FF_E = 7168
FD = 5632
B_DEV = 4
CAP = 2
TOKENS = 128
N_EP = 32


def block_scale(rng, extent, cuts, least, high):
    level, own = 1.0, jax.random.fold_in(rng, 6)
    for axis_at, blocks in cuts:
        draws = jnp.exp(jax.random.uniform(jax.random.fold_in(own, axis_at), (blocks,), jnp.float32, least / len(cuts), high / len(cuts)))
        level = level * jnp.repeat(draws, extent[axis_at] // blocks).reshape([-1 if axis == axis_at else 1 for axis in range(len(extent))])
    return level


def deal_out(key, own, number, rows, amount, top, reach, skew):
    order = jax.random.permutation(key, amount)
    crowded, usual = portions_of(amount, rows * top, reach, skew, True), portions_of(amount, rows * top, reach, skew, False)
    places = jnp.arange(amount)

    def named(sizes, rotation):
        used = int((sizes > 0).sum())
        fixed = max(1, used // 4)
        moved = fixed + (places - fixed + rotation * (used - fixed)) % max(1, amount - fixed)
        return jnp.zeros((amount,), jnp.int32).at[order[jnp.where(places < fixed, places, moved)]].set(jnp.asarray(sizes, jnp.int32))

    sizes = jnp.where(number % 4 == 0, named(crowded, number // 4), named(usual, number - number // 4 - 1))
    mixed = jax.random.permutation(jax.random.fold_in(own, 3), amount)
    donor, sink = mixed[0:amount // 2 * 2:2], mixed[1:amount // 2 * 2:2]
    room = jnp.minimum(sizes[donor] - 1, reach - sizes[sink]) // 2
    room = jnp.where((donor == order[0]) | (sink == order[0]) | (sizes[sink] == 0), 0, jnp.maximum(room, 0))
    moved = jax.random.randint(jax.random.fold_in(own, 4), (amount // 2,), 0, 1 << 20) % (room + 1)
    sizes = sizes.at[donor].add(-moved).at[sink].add(moved)
    members = jnp.searchsorted(jnp.cumsum(sizes), jnp.arange(rows * top), side="right").astype(jnp.int32)
    table = members.reshape(top, rows).T
    table = table[jax.random.permutation(jax.random.fold_in(own, 1), rows)]
    rotation = jax.random.randint(jax.random.fold_in(own, 2), (rows, 1), 0, top)
    return jnp.take_along_axis(table, (jnp.arange(top)[None, :] + rotation) % top, axis=1)


def portions_of(amount, total, reach, slope, full):
    weights = [(1 << 20) // math.isqrt(rank ** slope) + 1 for rank in range(1, amount + 1)]
    largest = reach if full else min(reach, max(-(-total // amount), total * weights[0] // sum(weights)))
    least = 1 if total - largest >= amount - 1 else 0
    holding, spare = [largest] + [least] * (amount - 1), total - largest - least * (amount - 1)
    while spare > 0:
        free = [i for i in range(1, amount) if holding[i] < largest] or [i for i in range(1, amount) if holding[i] < reach]
        mass, remaining = sum([weights[i] for i in free]), spare
        for i in free:
            addition = min(reach - holding[i], max(1, remaining * weights[i] // mass), spare)
            holding[i] = holding[i] + addition
            spare = spare - addition
    return np.array(holding)


def bell_draw(stream_key, shape, scale, limit, pieces=(), kind=jnp.bfloat16):
    level = block_scale(stream_key, shape, pieces, -0.22, 0.18) if pieces else 1.0
    result = jax.random.normal(stream_key, shape, jnp.float32) * scale * level
    return jnp.minimum(jnp.maximum(result, -limit), limit).astype(kind)


def setup_inputs(seed: int = 0) -> dict:
    keys = jax.random.split(jax.random.key(seed), 23)
    tokens = bell_draw(keys[0], (TOKENS, D), 1.0, 6.0, ((0, 32),))
    recurrent_state = bell_draw(keys[1], (TOKENS, HEADS, DK, DK), 0.5, 4.0, ((0, 32),), jnp.float32)
    query_weight = bell_draw(keys[2], (D, HGW), D ** -0.5, 0.125, ((1, 32),))
    forget_weight = bell_draw(keys[3], (D, HGW), D ** -0.5, 0.125, ((1, 32),))
    input_weight = bell_draw(keys[4], (D, HGW), D ** -0.5, 0.125, ((1, 32),))
    outgate_weight = bell_draw(keys[5], (D, HGW), D ** -0.5, 0.125, ((1, 32),))
    lower_bound = jnp.clip(jax.random.uniform(keys[6], (HGW,), jnp.float32, 0.0, 0.9), 0.0, 0.9)
    head_gain = jnp.clip(1.0 + 0.18 * jax.random.normal(keys[7], (DK,), jnp.float32), 0.1, 1.9)
    mixout_weight = bell_draw(keys[8], (HGW, D), HGW ** -0.5, 0.1875, ((1, 32),))
    first_gain = jnp.clip(1.0 + 0.18 * jax.random.normal(keys[9], (D,), jnp.float32), 0.1, 1.9)
    first_bias = bell_draw(keys[10], (D,), 0.3, 1.5, (), jnp.float32)
    router_weight = bell_draw(keys[11], (D, EXPERTS), D ** -0.5, 0.125)
    branch_vector = bell_draw(keys[12], (D,), D ** -0.5, 0.125)
    dense_gate_weight = bell_draw(keys[13], (D, FD), D ** -0.5, 0.125, ((1, 32),))
    dense_up_weight = bell_draw(keys[14], (D, FD), D ** -0.5, 0.125, ((1, 32),))
    dense_down_weight = bell_draw(keys[15], (FD, D), FD ** -0.5, 0.078125, ((0, 32),))
    expert_gate_weight = bell_draw(keys[16], (D, EXPERTS * FF_E), D ** -0.5, 0.125, ((1, 32),))
    expert_up_weight = bell_draw(keys[17], (D, EXPERTS * FF_E), D ** -0.5, 0.125, ((1, 32),))
    expert_down_weight = bell_draw(keys[18], (EXPERTS * FF_E, D), FF_E ** -0.5, 0.0625, ((0, 32),))
    second_gain = jnp.clip(1.0 + 0.18 * jax.random.normal(keys[19], (D,), jnp.float32), 0.1, 1.9)
    second_bias = bell_draw(keys[20], (D,), 0.3, 1.5, (), jnp.float32)
    routes_keys = jax.random.split(jax.random.fold_in(keys[21], 1), TOKENS // B_DEV)
    routes_turns = jax.random.permutation(jax.random.fold_in(keys[21], 3), TOKENS // B_DEV)
    routes = jax.vmap(lambda own, number: deal_out(jax.random.fold_in(keys[21], 2), own, number, B_DEV, EXPERTS, 2, CAP, 2))(routes_keys, routes_turns).reshape((TOKENS, 2))
    return dict(tokens=tokens, recurrent_state=recurrent_state, query_weight=query_weight, forget_weight=forget_weight, input_weight=input_weight, outgate_weight=outgate_weight, lower_bound=lower_bound, head_gain=head_gain, mixout_weight=mixout_weight, first_gain=first_gain, first_bias=first_bias, router_weight=router_weight, branch_vector=branch_vector, dense_gate_weight=dense_gate_weight, dense_up_weight=dense_up_weight, dense_down_weight=dense_down_weight, expert_gate_weight=expert_gate_weight, expert_up_weight=expert_up_weight, expert_down_weight=expert_down_weight, second_gain=second_gain, second_bias=second_bias, routes=routes)


ALPHA = 8.0 ** 0.25
NORM_EPS = 1e-05
HEAD_EPS = 1e-06

def layer_norm(mixture, gain, bias):
    center = lax.optimization_barrier(jnp.mean(mixture, axis=-1, keepdims=True))
    spread = lax.optimization_barrier(jnp.mean(jnp.square(mixture - center), axis=-1, keepdims=True))
    return (mixture - center) * lax.rsqrt(spread + NORM_EPS) * gain + bias

def recurrence(projected, state, lower_bound, head_gain):
    nseq, heads, width = (state.shape[0], state.shape[1], state.shape[2])
    query = projected[:, 0].astype(jnp.float32).reshape(nseq, heads, width)
    forget_in = projected[:, 1].astype(jnp.float32)
    value = projected[:, 2].astype(jnp.float32).reshape(nseq, heads, width)
    outgate = projected[:, 3].astype(jnp.float32)
    forget = (lower_bound + (1.0 - lower_bound) * jax.nn.sigmoid(forget_in)).reshape(nseq, heads, width)
    keyed = ((1.0 - lower_bound) * jax.nn.sigmoid(-forget_in)).reshape(nseq, heads, width)
    fresh = forget[..., None] * state + keyed[..., None] * value[:, :, None, :]
    read = jnp.einsum('bhkv,bhk->bhv', fresh, query, precision=lax.Precision.HIGHEST)
    scaled = read * lax.rsqrt(lax.optimization_barrier(jnp.mean(jnp.square(read), axis=-1, keepdims=True)) + HEAD_EPS) * head_gain
    mixed = (scaled.reshape(nseq, heads * width) * jax.nn.silu(outgate)).astype(jnp.bfloat16)
    return (mixed, fresh)

def reference(tokens, recurrent_state, query_weight, forget_weight, input_weight, outgate_weight, lower_bound, head_gain, mixout_weight, first_gain, first_bias, router_weight, branch_vector, dense_gate_weight, dense_up_weight, dense_down_weight, expert_gate_weight, expert_up_weight, expert_down_weight, second_gain, second_bias, routes):
    f32 = jnp.float32
    parts = [jnp.dot(tokens, weight, preferred_element_type=f32).astype(jnp.bfloat16) for weight in (query_weight, forget_weight, input_weight, outgate_weight)]
    projected = jnp.stack(parts, axis=1)
    mixed, new_state = recurrence(projected, recurrent_state, lower_bound, head_gain)
    mix_out = jnp.dot(mixed, mixout_weight, preferred_element_type=f32).astype(jnp.bfloat16)
    normed = layer_norm(ALPHA * tokens.astype(f32) + mix_out.astype(f32), first_gain, first_bias).astype(jnp.bfloat16)
    width = normed.shape[1]
    logits = jnp.dot(normed, router_weight, preferred_element_type=f32)
    expert_ids = jnp.arange(EXPERTS, dtype=jnp.int32)
    first_pick = routes[:, 0]
    second_pick = routes[:, 1]
    first_logit = lax.optimization_barrier(jnp.sum(jnp.where(first_pick[:, None] == expert_ids[None, :], logits, 0.0), axis=1))
    second_logit = lax.optimization_barrier(jnp.sum(jnp.where(second_pick[:, None] == expert_ids[None, :], logits, 0.0), axis=1))
    share = jax.nn.sigmoid(first_logit - second_logit)
    branch_gate = jax.nn.sigmoid(jnp.dot(normed, branch_vector, preferred_element_type=f32))
    dense_hidden = (jax.nn.silu(jnp.dot(normed, dense_gate_weight, preferred_element_type=f32)) * jnp.dot(normed, dense_up_weight, preferred_element_type=f32)).astype(jnp.bfloat16)
    channel = branch_gate[:, None] * jnp.dot(dense_hidden, dense_down_weight, preferred_element_type=f32)
    blocks = normed.reshape(N_EP, B_DEV, width).astype(f32)
    slot_ids = jnp.arange(CAP, dtype=jnp.int32)
    for expert in range(EXPERTS):
        on_first = first_pick == expert
        on_second = second_pick == expert
        token_weight = share * on_first.astype(f32) + (1.0 - share) * on_second.astype(f32)
        hits = (on_first | on_second).astype(jnp.int32).reshape(N_EP, B_DEV)
        ranks = jnp.cumsum(hits, axis=1) - 1
        select = ((ranks[:, None, :] == slot_ids[None, :, None]) & (hits[:, None, :] > 0)).astype(f32)
        slot_rows = jnp.einsum('sci,sid->scd', select, blocks, precision=lax.Precision.HIGHEST)
        slot_rows = slot_rows.astype(jnp.bfloat16).reshape(N_EP * CAP, width)
        low = expert * FF_E
        gate_part = jnp.dot(slot_rows, expert_gate_weight[:, low:low + FF_E], preferred_element_type=f32)
        up_part = jnp.dot(slot_rows, expert_up_weight[:, low:low + FF_E], preferred_element_type=f32)
        hidden = (jax.nn.silu(gate_part) * up_part).astype(jnp.bfloat16)
        slot_out = jnp.dot(hidden, expert_down_weight[low:low + FF_E, :], preferred_element_type=f32)
        slot_out = slot_out.reshape(N_EP, CAP, width)
        back = jnp.einsum('sci,scd->sid', select, slot_out, precision=lax.Precision.HIGHEST)
        channel = channel + back.reshape(N_EP * B_DEV, width) * token_weight[:, None]
    output = layer_norm(ALPHA * normed.astype(f32) + channel, second_gain, second_bias).astype(jnp.bfloat16)
    return (output, new_state)
```

```python
import jax
import jax.numpy as jnp
from jax import lax
from jax.sharding import PartitionSpec as P

ALPHA = 8.0**0.25
NORM_EPS = 1e-05
HEAD_EPS = 1e-06


def layer_norm(mixture, gain, bias):
    center = jnp.mean(mixture, axis=-1, keepdims=True)
    spread = jnp.mean(jnp.square(mixture - center), axis=-1, keepdims=True)
    return (mixture - center) * lax.rsqrt(spread + NORM_EPS) * gain + bias


def recurrence(projected, state, lower_bound, head_gain):
    nseq, heads, width = (state.shape[0], state.shape[1], state.shape[2])
    query = projected[:, 0].astype(jnp.float32).reshape(nseq, heads, width)
    forget_in = projected[:, 1].astype(jnp.float32)
    value = projected[:, 2].astype(jnp.float32).reshape(nseq, heads, width)
    outgate = projected[:, 3].astype(jnp.float32)
    forget = (lower_bound + (1.0 - lower_bound) * jax.nn.sigmoid(forget_in)).reshape(
        nseq, heads, width
    )
    keyed = ((1.0 - lower_bound) * jax.nn.sigmoid(-forget_in)).reshape(nseq, heads, width)
    fresh = forget[..., None] * state + keyed[..., None] * value[:, :, None, :]
    read = jnp.einsum("bhkv,bhk->bhv", fresh, query, precision=lax.Precision.HIGHEST)
    scaled = (
        read * lax.rsqrt(jnp.mean(jnp.square(read), axis=-1, keepdims=True) + HEAD_EPS) * head_gain
    )
    mixed = (scaled.reshape(nseq, heads * width) * jax.nn.silu(outgate)).astype(jnp.bfloat16)
    return (mixed, fresh)


def gather_all(block):
    devices = lax.axis_size("ep")
    copies = jnp.broadcast_to(block[None], (devices,) + block.shape)
    return lax.all_to_all(copies, "ep", split_axis=0, concat_axis=0, tiled=True)


def expert_weight(logits, routes, expert):
    expert_ids = jnp.arange(logits.shape[1], dtype=jnp.int32)
    first_logit = jnp.sum(jnp.where(routes[:, 0:1] == expert_ids[None, :], logits, 0.0), axis=1)
    second_logit = jnp.sum(jnp.where(routes[:, 1:2] == expert_ids[None, :], logits, 0.0), axis=1)
    share = jax.nn.sigmoid(first_logit - second_logit)
    return jnp.where(
        routes[:, 0] == expert, share, jnp.where(routes[:, 1] == expert, 1.0 - share, 0.0)
    )


def gated_hidden(rows, gate_weight, up_weight):
    f32 = jnp.float32
    return (
        jax.nn.silu(jnp.dot(rows, gate_weight, preferred_element_type=f32))
        * jnp.dot(rows, up_weight, preferred_element_type=f32)
    ).astype(jnp.bfloat16)


def per_device(
    tokens,
    recurrent_state,
    query_weight,
    forget_weight,
    input_weight,
    outgate_weight,
    lower_bound,
    head_gain,
    mixout_weight,
    first_gain,
    first_bias,
    router_weight,
    branch_vector,
    dense_gate_weight,
    dense_up_weight,
    dense_down_weight,
    expert_gate_weight,
    expert_up_weight,
    expert_down_weight,
    second_gain,
    second_bias,
    routes,
):
    f32 = jnp.float32
    bf16 = jnp.bfloat16
    devices = lax.axis_size("ep")
    nseq, width = tokens.shape
    own_cols = query_weight.shape[1]
    experts = router_weight.shape[1]
    own_index = lax.axis_index("ep")
    row_start = own_index * nseq
    own_expert = own_index // (devices // experts)

    stacked = jnp.concatenate([query_weight, forget_weight, input_weight, outgate_weight], axis=1)
    tokens_all = gather_all(tokens).reshape(devices * nseq, width)
    gathered = jnp.dot(tokens_all, stacked, preferred_element_type=f32).astype(bf16)
    owned = lax.all_to_all(gathered, "ep", split_axis=0, concat_axis=1, tiled=True)
    projected = (
        owned.reshape(nseq, devices, 4, own_cols)
        .transpose(0, 2, 1, 3)
        .reshape(nseq, 4, devices * own_cols)
    )
    mixed, new_state = recurrence(projected, recurrent_state, lower_bound, head_gain)

    mixed_all = gather_all(mixed).reshape(devices * nseq, -1)
    mix_rows = lax.dot_general(
        mixout_weight, mixed_all, (((0,), (1,)), ((), ())), preferred_element_type=f32
    ).astype(bf16)
    mix_out = gather_all(mix_rows).reshape(width, devices * nseq).T
    normed_all = layer_norm(
        ALPHA * tokens_all.astype(f32) + mix_out.astype(f32), first_gain, first_bias
    ).astype(bf16)
    own_normed = lax.dynamic_slice_in_dim(normed_all, row_start, nseq, 0)

    logits = jnp.dot(normed_all, router_weight, preferred_element_type=f32)
    weight = expert_weight(logits, routes, own_expert)
    branch_gate = jax.nn.sigmoid(jnp.dot(normed_all, branch_vector, preferred_element_type=f32))
    dense_hidden = gated_hidden(normed_all, dense_gate_weight, dense_up_weight)
    hidden = gated_hidden(normed_all, expert_gate_weight, expert_up_weight)
    partial = branch_gate[:, None] * jnp.dot(
        dense_hidden, dense_down_weight, preferred_element_type=f32
    ) + weight[:, None] * jnp.dot(hidden, expert_down_weight, preferred_element_type=f32)
    returned = lax.all_to_all(
        partial.astype(bf16).reshape(devices, nseq, width),
        "ep",
        split_axis=0,
        concat_axis=0,
        tiled=True,
    )
    channel = jnp.sum(returned.astype(f32), axis=0)
    output = layer_norm(ALPHA * own_normed.astype(f32) + channel, second_gain, second_bias).astype(
        bf16
    )
    return (output, new_state)


def solution(mesh):
    return jax.shard_map(
        per_device,
        mesh=mesh,
        in_specs=(
            P("ep", None),
            P("ep", None, None, None),
            P(None, "ep"),
            P(None, "ep"),
            P(None, "ep"),
            P(None, "ep"),
            P(),
            P(),
            P(None, "ep"),
            P(),
            P(),
            P(),
            P(),
            P(None, "ep"),
            P(None, "ep"),
            P("ep", None),
            P(None, "ep"),
            P(None, "ep"),
            P("ep", None),
            P(),
            P(),
            P(),
        ),
        out_specs=(P("ep", None), P("ep", None, None, None)),
        check_vma=False,
    )
```

```python
import jax
import jax.numpy as jnp
from jax import lax
from jax.experimental import pallas as pl
from jax.experimental.pallas import tpu as pltpu
from jax.sharding import PartitionSpec as P

ALPHA = 8.0**0.25
NORM_EPS = 1e-05
HEAD_EPS = 1e-06


def layer_norm(mixture, gain, bias):
    center = jnp.mean(mixture, axis=-1, keepdims=True)
    spread = jnp.mean(jnp.square(mixture - center), axis=-1, keepdims=True)
    return (mixture - center) * lax.rsqrt(spread + NORM_EPS) * gain + bias


def recurrence(projected, state, lower_bound, head_gain):
    nseq, heads, width = (state.shape[0], state.shape[1], state.shape[2])
    query = projected[:, 0].astype(jnp.float32).reshape(nseq, heads, width)
    forget_in = projected[:, 1].astype(jnp.float32)
    value = projected[:, 2].astype(jnp.float32).reshape(nseq, heads, width)
    outgate = projected[:, 3].astype(jnp.float32)
    forget = (lower_bound + (1.0 - lower_bound) * jax.nn.sigmoid(forget_in)).reshape(
        nseq, heads, width
    )
    keyed = ((1.0 - lower_bound) * jax.nn.sigmoid(-forget_in)).reshape(nseq, heads, width)
    fresh = forget[..., None] * state + keyed[..., None] * value[:, :, None, :]
    read = jnp.einsum("bhkv,bhk->bhv", fresh, query, precision=lax.Precision.HIGHEST)
    scaled = (
        read * lax.rsqrt(jnp.mean(jnp.square(read), axis=-1, keepdims=True) + HEAD_EPS) * head_gain
    )
    mixed = (scaled.reshape(nseq, heads * width) * jax.nn.silu(outgate)).astype(jnp.bfloat16)
    return (mixed, fresh)


def gather_all(block):
    devices = lax.axis_size("ep")
    copies = jnp.broadcast_to(block[None], (devices,) + block.shape)
    return lax.all_to_all(copies, "ep", split_axis=0, concat_axis=0, tiled=True)


def hidden_block(extent):
    for size in (256, 128):
        if extent % size == 0:
            return size
    return extent


def channel_kernel(
    mix_ref,
    tokens_ref,
    gain_ref,
    bias_ref,
    router_ref,
    pick_ref,
    first_ref,
    second_ref,
    dense_gate_hbm,
    dense_up_hbm,
    dense_down_hbm,
    gate_hbm,
    up_hbm,
    down_hbm,
    partial_ref,
    normed_ref,
    dense_gate,
    dense_up,
    dense_down,
    gate,
    up,
    down,
    acc_ref,
    sems,
    dense_sems,
):
    f32 = jnp.float32
    bf16 = jnp.bfloat16
    extent = gate_hbm.shape[1]
    block = hidden_block(extent)
    spans = [pl.ds(at, block) for at in range(0, extent, block)]
    copies = []
    for step, span in enumerate(spans):
        copies.append(
            (
                pltpu.make_async_copy(gate_hbm.at[:, span], gate.at[:, span], sems.at[0, step]),
                pltpu.make_async_copy(up_hbm.at[:, span], up.at[:, span], sems.at[1, step]),
                pltpu.make_async_copy(down_hbm.at[span, :], down.at[span, :], sems.at[2, step]),
            )
        )
    dense_copies = (
        pltpu.make_async_copy(dense_gate_hbm, dense_gate, dense_sems.at[0]),
        pltpu.make_async_copy(dense_up_hbm, dense_up, dense_sems.at[1]),
        pltpu.make_async_copy(dense_down_hbm, dense_down, dense_sems.at[2]),
    )
    for copy in dense_copies:
        copy.start()
    for group in copies:
        for copy in group:
            copy.start()

    mixture = ALPHA * tokens_ref[...].astype(f32) + mix_ref[...].astype(f32).T
    normed_ref[...] = layer_norm(mixture, gain_ref[...], bias_ref[...]).astype(bf16)
    last = (((1,), (1,)), ((), ()))
    scores = lax.dot_general(normed_ref[...], router_ref[...], last, preferred_element_type=f32)
    branch_gate = jax.nn.sigmoid(scores[:, -1:])
    share = jax.nn.sigmoid(jnp.sum(scores * pick_ref[...], axis=1, keepdims=True))
    weight = first_ref[...] * share + second_ref[...] * (1.0 - share)

    for copy in dense_copies:
        copy.wait()
    rows = normed_ref[...]
    dense_hidden = jax.nn.silu(
        lax.dot_general(rows, dense_gate[...], last, preferred_element_type=f32)
    ) * lax.dot_general(rows, dense_up[...], last, preferred_element_type=f32)
    dense_part = jnp.dot(dense_hidden.astype(bf16), dense_down[...], preferred_element_type=f32)
    acc_ref[...] = branch_gate * dense_part

    for group, span in zip(copies, spans):
        for copy in group:
            copy.wait()
        rows = normed_ref[...]
        hidden = jax.nn.silu(
            jnp.dot(rows, gate[:, span], preferred_element_type=f32)
        ) * jnp.dot(rows, up[:, span], preferred_element_type=f32)
        acc_ref[...] += weight * jnp.dot(
            hidden.astype(bf16), down[span, :], preferred_element_type=f32
        )
    held = partial_ref.shape[1]
    for device in range(partial_ref.shape[0]):
        partial_ref[device] = acc_ref[device * held : (device + 1) * held, :].astype(bf16)


def channel_stage(nseq, mix_rows, tokens_all, gain, bias, router, pick, first, second, *weights):
    count, width = tokens_all.shape
    bf16 = jnp.bfloat16
    steps = weights[3].shape[1] // hidden_block(weights[3].shape[1])
    whole = pl.BlockSpec(memory_space=pltpu.VMEM)
    return pl.pallas_call(
        channel_kernel,
        out_shape=[
            jax.ShapeDtypeStruct((count // nseq, nseq, width), bf16),
            jax.ShapeDtypeStruct((count, width), bf16),
        ],
        in_specs=[whole] * 8 + [pl.BlockSpec(memory_space=pl.ANY)] * 6,
        out_specs=[whole] * 2,
        scratch_shapes=[pltpu.VMEM(w.shape, bf16) for w in weights]
        + [
            pltpu.VMEM((count, width), jnp.float32),
            pltpu.SemaphoreType.DMA((3, steps)),
            pltpu.SemaphoreType.DMA((3,)),
        ],
        compiler_params=pltpu.CompilerParams(vmem_limit_bytes=44 * 1024 * 1024),
        name="channel",
    )(mix_rows, tokens_all, gain, bias, router, pick, first, second, *weights)


def per_device(
    tokens,
    recurrent_state,
    query_weight,
    forget_weight,
    input_weight,
    outgate_weight,
    lower_bound,
    head_gain,
    mixout_weight,
    first_gain,
    first_bias,
    router_weight,
    branch_vector,
    dense_gate_weight,
    dense_up_weight,
    dense_down_weight,
    expert_gate_weight,
    expert_up_weight,
    expert_down_weight,
    second_gain,
    second_bias,
    routes,
):
    f32 = jnp.float32
    bf16 = jnp.bfloat16
    devices = lax.axis_size("ep")
    nseq, width = tokens.shape
    own_cols = query_weight.shape[1]
    experts = router_weight.shape[1]
    own_index = lax.axis_index("ep")
    row_start = own_index * nseq
    own_expert = own_index // (devices // experts)

    stacked = jnp.concatenate([query_weight, forget_weight, input_weight, outgate_weight], axis=1)
    tokens_all = gather_all(tokens).reshape(devices * nseq, width)
    gathered = jnp.dot(tokens_all, stacked, preferred_element_type=f32).astype(bf16)
    owned = lax.all_to_all(gathered, "ep", split_axis=0, concat_axis=1, tiled=True)
    projected = (
        owned.reshape(nseq, devices, 4, own_cols)
        .transpose(0, 2, 1, 3)
        .reshape(nseq, 4, devices * own_cols)
    )
    mixed, new_state = recurrence(projected, recurrent_state, lower_bound, head_gain)

    mixed_all = gather_all(mixed).reshape(devices * nseq, -1)
    mix_rows = lax.dot_general(
        mixout_weight, mixed_all, (((0,), (1,)), ((), ())), preferred_element_type=f32
    ).astype(bf16)
    mix_out = gather_all(mix_rows).reshape(width, devices * nseq)

    columns = jnp.arange(2 * experts, dtype=jnp.int32)[None, :]
    router = jnp.concatenate(
        [router_weight.T, jnp.zeros((experts - 1, width), bf16), branch_vector[None, :]], axis=0
    )
    pick = (routes[:, 0:1] == columns).astype(f32) - (routes[:, 1:2] == columns).astype(f32)
    first = (routes[:, 0:1] == own_expert).astype(f32)
    second = (routes[:, 1:2] == own_expert).astype(f32)
    partial, normed_all = channel_stage(
        nseq,
        mix_out,
        tokens_all,
        first_gain[None, :],
        first_bias[None, :],
        router,
        pick,
        first,
        second,
        dense_gate_weight.T,
        dense_up_weight.T,
        dense_down_weight,
        expert_gate_weight,
        expert_up_weight,
        expert_down_weight,
    )
    own_normed = lax.dynamic_slice_in_dim(normed_all, row_start, nseq, 0)
    returned = lax.all_to_all(
        partial,
        "ep",
        split_axis=0,
        concat_axis=0,
        tiled=True,
    )
    channel = jnp.sum(returned.astype(f32), axis=0)
    output = layer_norm(ALPHA * own_normed.astype(f32) + channel, second_gain, second_bias).astype(
        bf16
    )
    return (output, new_state)


def solution(mesh):
    return jax.shard_map(
        per_device,
        mesh=mesh,
        in_specs=(
            P("ep", None),
            P("ep", None, None, None),
            P(None, "ep"),
            P(None, "ep"),
            P(None, "ep"),
            P(None, "ep"),
            P(),
            P(),
            P(None, "ep"),
            P(),
            P(),
            P(),
            P(),
            P(None, "ep"),
            P(None, "ep"),
            P("ep", None),
            P(None, "ep"),
            P(None, "ep"),
            P("ep", None),
            P(),
            P(),
            P(),
        ),
        out_specs=(P("ep", None), P("ep", None, None, None)),
        check_vma=False,
    )
```
